32 devices in a mesh: rep: 2 (over x), fs: 8 (over z, y), tp: 2 (over core).
Axes of the slice: x: 2, y: 2, z: 4, core: 2. Of those that a mesh axis runs over, the one named last changes fastest.
Arguments:
- stream_in: bfloat16 [16, 768, 2048], P(('rep', 'fs'), None, 'tp'), may hold values from -6 to 6
- mix_gain: float32 [2048], replicated, may hold values from 0.1 to 1.9
- lin_weight: bfloat16 [2048, 2048], P('fs', 'tp'), may hold values from -0.125 to 0.125
- branch_weight: bfloat16 [2048, 2048], P('fs', 'tp'), may hold values from -0.125 to 0.125
- lin_taps: float32 [4, 2048], P(None, 'tp'), may hold values from -3 to 3
- rate_blocks: bfloat16 [16, 128, 128], P('tp'), may hold values from -0.5 to 0.5
- admit_blocks: bfloat16 [16, 128, 128], P('tp'), may hold values from -0.5 to 0.5
- decay_logit: float32 [2048], P('tp'), may hold values from 3.5 to 9
- mix_out_gain: float32 [2048], P('tp'), may hold values from 0.1 to 1.9
- out_weight: bfloat16 [2048, 2048], P('tp', 'fs'), may hold values from -0.125 to 0.125
- ffn_gain: float32 [2048], replicated, may hold values from 0.1 to 1.9
- gate_weight: bfloat16 [2048, 2816], P('fs', 'tp'), may hold values from -0.125 to 0.125
- up_weight: bfloat16 [2048, 2816], P('fs', 'tp'), may hold values from -0.125 to 0.125
- gate_taps: float32 [3, 2816], P(None, 'tp'), may hold values from -3 to 3
- up_taps: float32 [3, 2816], P(None, 'tp'), may hold values from -3 to 3
- down_weight: bfloat16 [2816, 2048], P('tp', 'fs'), may hold values from -0.109375 to 0.109375
Outputs:
- stream_out: bfloat16 [16, 768, 2048], P(('rep', 'fs'), None, 'tp')
The draws below stay inside these ranges and needn't reach their ends.
All inputs are finite; a program needn't handle non-finite values.
Results may differ from the reference program's by a relative error of at most 0.018.
Values may be sent and summed in bfloat16 or wider, within the bound.
A program may use at most 128 MiB of HBM per device.

```python
import jax
import jax.numpy as jnp
from jax import lax

D = 2048
HD = 128
BLOCKS = 16
FF = 2816
LEN = 768
LRU = 2048
SEQS = 16
N_TP = 2


def steps_of(rng, dims, split, smallest, top_value):
    level = 1.0
    for axis_at, parts in split:
        heights = jax.random.uniform(jax.random.fold_in(jax.random.fold_in(rng, 6), axis_at), (parts,), jnp.float32, smallest / len(split), top_value / len(split))
        level = level * jnp.repeat(jnp.exp(heights), dims[axis_at] // parts).reshape((-1,) + (1,) * (len(dims) - 1 - axis_at))
    return level


def scatter_about(rng, dims, deviation, limit, cuts=(), held_as=jnp.bfloat16):
    level = steps_of(rng, dims, cuts, -0.22, 0.18) if cuts else 1.0
    array = jax.random.normal(rng, dims, jnp.float32) * deviation * level
    return jnp.minimum(jnp.maximum(array, -limit), limit).astype(held_as)


def setup_inputs(seed: int = 0) -> dict:
    streams_of = jax.random.split(jax.random.key(seed), 17)
    return {
        "stream_in": scatter_about(streams_of[0], (SEQS, LEN, D), 1.0, 6.0, ((0, 16), (2, 2))),
        "mix_gain": jnp.clip(1.0 + 0.18 * jax.random.normal(streams_of[1], (D,), jnp.float32), 0.1, 1.9),
        "lin_weight": scatter_about(streams_of[2], (D, LRU), D ** -0.5, 0.125, ((0, 8), (1, 2))),
        "branch_weight": scatter_about(streams_of[3], (D, LRU), D ** -0.5, 0.125, ((0, 8), (1, 2))),
        "lin_taps": scatter_about(streams_of[4], (4, LRU), 0.5, 3.0, ((1, 2),), jnp.float32),
        "rate_blocks": scatter_about(streams_of[5], (BLOCKS, HD, HD), HD ** -0.5, 0.5, ((0, 2),)),
        "admit_blocks": scatter_about(streams_of[6], (BLOCKS, HD, HD), HD ** -0.5, 0.5, ((0, 2),)),
        "decay_logit": jnp.clip(3.5 + 5.5 * jax.random.uniform(streams_of[7], (LRU,), jnp.float32) ** steps_of(streams_of[7], (LRU,), ((0, 2),), -0.2, 0.2), 3.5, 9.0),
        "mix_out_gain": jnp.clip(1.0 + 0.18 * jax.random.normal(streams_of[8], (LRU,), jnp.float32), 0.1, 1.9),
        "out_weight": scatter_about(streams_of[9], (LRU, D), LRU ** -0.5, 0.125, ((0, 2), (1, 8))),
        "ffn_gain": jnp.clip(1.0 + 0.18 * jax.random.normal(streams_of[10], (D,), jnp.float32), 0.1, 1.9),
        "gate_weight": scatter_about(streams_of[11], (D, FF), D ** -0.5, 0.125, ((0, 8), (1, 2))),
        "up_weight": scatter_about(streams_of[12], (D, FF), D ** -0.5, 0.125, ((0, 8), (1, 2))),
        "gate_taps": scatter_about(streams_of[13], (3, FF), 0.6, 3.0, ((1, 2),), jnp.float32),
        "up_taps": scatter_about(streams_of[14], (3, FF), 0.6, 3.0, ((1, 2),), jnp.float32),
        "down_weight": scatter_about(streams_of[15], (FF, D), FF ** -0.5, 0.109375, ((0, 2), (1, 8))),
    }


EPS = 1e-06
GATE_SCALE = 8.0

def norm_rows(values, scales):
    mean_sq = lax.optimization_barrier(jnp.mean(values * values, axis=-1, keepdims=True))
    return values * lax.rsqrt(mean_sq + EPS) * scales

def causal_filter(values, kernel):
    kernel_len = kernel.shape[0]
    seq_len = values.shape[0]
    padded = jnp.pad(values, ((kernel_len - 1, 0), (0, 0)))
    summed = padded[0:seq_len] * kernel[0]
    for offset in range(1, kernel_len):
        summed = summed + padded[offset:offset + seq_len] * kernel[offset]
    return summed

def chain_combine(earlier, later):
    return (earlier[0] * later[0], later[0] * earlier[1] + later[1])

def split_product(left, right):
    group = left.shape[1] // N_TP
    summed = jnp.zeros((left.shape[0], right.shape[1]), jnp.float32)
    for column_part in range(N_TP):
        partial_value = jnp.dot(left[:, column_part * group:(column_part + 1) * group], right[column_part * group:(column_part + 1) * group], preferred_element_type=jnp.float32)
        partial_value = lax.optimization_barrier(partial_value.astype(jnp.bfloat16))
        summed = summed + partial_value.astype(jnp.float32)
    return summed

def reference(stream_in, mix_gain, lin_weight, branch_weight, lin_taps, rate_blocks, admit_blocks, decay_logit, mix_out_gain, out_weight, ffn_gain, gate_weight, up_weight, gate_taps, up_taps, down_weight):

    def one_sequence(sequence):
        stream = sequence.astype(jnp.float32)
        normed = norm_rows(stream, mix_gain).astype(jnp.bfloat16)
        linear = jnp.dot(normed, lin_weight, preferred_element_type=jnp.float32).astype(jnp.bfloat16)
        branch = jnp.dot(normed, branch_weight, preferred_element_type=jnp.float32).astype(jnp.bfloat16)
        filtered = causal_filter(linear.astype(jnp.float32), lin_taps)
        blocks = filtered.astype(jnp.bfloat16).astype(jnp.float32).reshape(LEN, BLOCKS, HD)
        rate_gate = jax.nn.sigmoid(jnp.einsum('lbi,bij->lbj', blocks, rate_blocks.astype(jnp.float32)).reshape(LEN, BLOCKS * HD))
        admitted = jax.nn.sigmoid(jnp.einsum('lbi,bij->lbj', blocks, admit_blocks.astype(jnp.float32)).reshape(LEN, BLOCKS * HD))
        log_decay = -GATE_SCALE * rate_gate * jax.nn.softplus(-decay_logit)
        decay = jnp.exp(log_decay)
        driven = jnp.sqrt(-jnp.expm1(2.0 * log_decay)) * admitted * filtered
        _, states = lax.associative_scan(chain_combine, (decay, driven), axis=0)
        gated = (states * jax.nn.gelu(branch.astype(jnp.float32))).reshape(LEN, BLOCKS, HD)
        gated = gated * lax.rsqrt(lax.optimization_barrier(jnp.mean(gated * gated, axis=-1, keepdims=True)) + EPS)
        mixed = (gated.reshape(LEN, BLOCKS * HD) * mix_out_gain).astype(jnp.bfloat16)
        middle = (stream + split_product(mixed, out_weight)).astype(jnp.bfloat16)
        normed2 = norm_rows(middle.astype(jnp.float32), ffn_gain).astype(jnp.bfloat16)
        gate_pre = jnp.dot(normed2, gate_weight, preferred_element_type=jnp.float32).astype(jnp.bfloat16)
        up_pre = jnp.dot(normed2, up_weight, preferred_element_type=jnp.float32).astype(jnp.bfloat16)
        gate_conv = causal_filter(gate_pre.astype(jnp.float32), gate_taps)
        up_conv = causal_filter(up_pre.astype(jnp.float32), up_taps)
        hidden = (jax.nn.silu(gate_conv) * up_conv).astype(jnp.bfloat16)
        return (middle.astype(jnp.float32) + split_product(hidden, down_weight)).astype(jnp.bfloat16)
    return lax.map(one_sequence, stream_in)
```

```python
import functools

import jax
import jax.numpy as jnp
from jax import lax
from jax.experimental import pallas as pl
from jax.experimental.pallas import tpu as pltpu
from jax.sharding import PartitionSpec as P

EPS = 1e-06
GATE_SCALE = 8.0
CHAIN_LIMIT = 8


def ring_order(n):
    return [i for i in range(0, n, 2)] + [i for i in range(1, n, 2)][::-1]


def owner_at(pos, n):
    pos = lax.rem(pos + 2 * n, n)
    half = (n + 1) // 2
    return jnp.where(pos < half, 2 * pos, 2 * (n - 1 - pos) + 1)


def chain_gather(shard, reps, n, sign, name):
    order = ring_order(n)
    place = {f: p for p, f in enumerate(order)}
    f = lax.axis_index("fs")
    rep = lax.axis_index("rep")
    me = jnp.where(f % 2 == 0, f // 2, n - 1 - f // 2)

    def step(direction):
        return [
            (r * n + g, r * n + order[(place[g] + direction(r)) % n])
            for r in range(reps)
            for g in range(n)
        ]

    if reps == 2:
        main_dir = lambda r: sign if r == 0 else -sign
        heading = jnp.where(rep == 0, sign, -sign)
        short = max((n // 2 - 1) // 3, min(1, n // 2 - 1))
    else:
        main_dir = lambda r: sign
        heading = sign
        short = n // 2 - 1
    other_dir = lambda r: -main_dir(r)
    swap = [(r * n + g, (1 - r) * n + g) for r in range(reps) for g in range(n)]
    out = [("own", f, shard)]
    held = shard
    back = shard
    with jax.named_scope(name):
        for k in range(1, n // 2 + 1):
            with jax.named_scope("m" + str(k)):
                held = lax.ppermute(held, ("rep", "fs"), step(main_dir))
            out.append(("m" + str(k), owner_at(me - heading * k, n), held))
            if k <= n // 2 - 1:
                if k <= short:
                    with jax.named_scope("o" + str(k)):
                        back = lax.ppermute(back, ("rep", "fs"), step(other_dir))
                    out.append(("o" + str(k), owner_at(me + heading * k, n), back))
                else:
                    with jax.named_scope("x" + str(k)):
                        far = lax.ppermute(held, ("rep", "fs"), swap)
                    out.append(("x" + str(k), owner_at(me + heading * k, n), far))
    return out


def tie(values, gathers, tags):
    if not any(entry[0] in tags for g in gathers for entry in g):
        return values
    picked = [(g, i) for g in gathers for i, entry in enumerate(g) if entry[0] in tags]
    tied, shards = lax.optimization_barrier((values, [g[i][2] for g, i in picked]))
    for (g, i), shard in zip(picked, shards):
        g[i] = (g[i][0], g[i][1], shard)
    return tied


def shift_rows(x, d, fill):
    rows = lax.broadcasted_iota(jnp.int32, x.shape, 0)
    return jnp.where(rows < d, fill, pltpu.roll(x, d, 0))


def mixer_body(lin_ref, br_ref, taps_ref, rate_ref, admit_ref, slope_ref, gain_ref, o_ref, a_ref, b_ref):
    length, width = lin_ref.shape
    hd = rate_ref.shape[1]
    linear = lin_ref[...].astype(jnp.float32)
    kernel_len = taps_ref.shape[0]
    filtered = linear * taps_ref[kernel_len - 1 : kernel_len]
    for d in range(1, kernel_len):
        filtered = filtered + shift_rows(linear, d, 0.0) * taps_ref[kernel_len - 1 - d : kernel_len - d]
    narrow = filtered.astype(jnp.bfloat16)
    for j in range(width // hd):
        cols = slice(j * hd, (j + 1) * hd)
        piece = narrow[:, cols]
        rate = jax.nn.sigmoid(jnp.dot(piece, rate_ref[j], preferred_element_type=jnp.float32))
        admit = jax.nn.sigmoid(jnp.dot(piece, admit_ref[j], preferred_element_type=jnp.float32))
        log_decay = rate * slope_ref[:, cols]
        u = 2.0 * log_decay
        decay = jnp.exp(log_decay)
        poly = 1.0 + u * (1.0 / 7.0)
        for c in (6.0, 5.0, 4.0, 3.0, 2.0):
            poly = 1.0 + u * (1.0 / c) * poly
        loss = jnp.where(u > -0.35, -u * poly, 1.0 - decay * decay)
        a = decay
        b = jnp.sqrt(loss) * admit * filtered[:, cols]
        sub = lax.broadcasted_iota(jnp.int32, a.shape, 0) % 8
        for d in (1, 2, 4):
            keep = sub >= d
            pa = jnp.where(keep, pltpu.roll(a, d, 0), 1.0)
            pb = jnp.where(keep, pltpu.roll(b, d, 0), 0.0)
            b = a * pb + b
            a = a * pa
        a_ref[:, cols] = a
        b_ref[:, cols] = b

    def advance(t, carry):
        rows = pl.ds(pl.multiple_of(t * 8, 8), 8)
        s = a_ref[rows, :] * carry + b_ref[rows, :]
        b_ref[rows, :] = s
        return s[7:8, :]

    lax.fori_loop(0, length // 8, advance, jnp.zeros((1, width), jnp.float32), unroll=8)
    for j in range(width // hd):
        cols = slice(j * hd, (j + 1) * hd)
        gated = b_ref[:, cols] * jax.nn.gelu(br_ref[:, cols].astype(jnp.float32))
        scale = lax.rsqrt(jnp.mean(gated * gated, axis=-1, keepdims=True) + EPS)
        o_ref[:, cols] = (gated * scale * gain_ref[:, cols]).astype(o_ref.dtype)


def mixer(linear, branch, taps, rate_blocks, admit_blocks, slope, gain):
    length, channels = linear.shape
    hd = rate_blocks.shape[1]
    per = 2 if rate_blocks.shape[0] % 2 == 0 else 1
    width = per * hd
    wide = pl.BlockSpec((length, width), lambda i: (0, i))
    row = pl.BlockSpec((1, width), lambda i: (0, i))
    blk = pl.BlockSpec((per, hd, hd), lambda i: (i, 0, 0))
    return pl.pallas_call(
        mixer_body,
        grid=(channels // width,),
        in_specs=[wide, wide, pl.BlockSpec((taps.shape[0], width), lambda i: (0, i)), blk, blk, row, row],
        out_specs=wide,
        out_shape=jax.ShapeDtypeStruct((length, channels), jnp.bfloat16),
        scratch_shapes=[pltpu.VMEM((length, width), jnp.float32), pltpu.VMEM((length, width), jnp.float32)],
        cost_estimate=pl.CostEstimate(flops=length * channels * 20000, bytes_accessed=length * channels * 6, transcendentals=0),
        name="mixer",
    )(linear, branch, taps, rate_blocks, admit_blocks, slope, gain)


def ffn_body(g_ref, u_ref, gt_ref, ut_ref, o_ref):
    def conv(ref, taps):
        x = ref[...].astype(jnp.float32)
        n = taps.shape[0]
        y = x * taps[n - 1 : n]
        for d in range(1, n):
            y = y + shift_rows(x, d, 0.0) * taps[n - 1 - d : n - d]
        return y

    o_ref[...] = (jax.nn.silu(conv(g_ref, gt_ref)) * conv(u_ref, ut_ref)).astype(o_ref.dtype)


def ffn_gate(gate_pre, up_pre, gate_taps, up_taps):
    length, units = gate_pre.shape
    width = 128
    wide = pl.BlockSpec((length, width), lambda i: (0, i))
    tap = pl.BlockSpec((gate_taps.shape[0], width), lambda i: (0, i))
    return pl.pallas_call(
        ffn_body,
        grid=(units // width,),
        in_specs=[wide, wide, tap, tap],
        out_specs=wide,
        out_shape=jax.ShapeDtypeStruct((length, units), jnp.bfloat16),
        cost_estimate=pl.CostEstimate(flops=length * units * 8000, bytes_accessed=length * units * 6, transcendentals=0),
        name="ffn_gate",
    )(gate_pre, up_pre, gate_taps, up_taps)


def by_rows(blocks, gathered):
    if gathered[0][0] == "all":
        left = blocks.transpose(1, 0, 2).reshape(blocks.shape[1], -1)
        return jnp.dot(left, gathered[0][2], preferred_element_type=jnp.float32).astype(jnp.bfloat16)
    total = None
    for _, owner, shard in gathered:
        part = jnp.dot(
            lax.dynamic_index_in_dim(blocks, owner, 0, keepdims=False), shard, preferred_element_type=jnp.float32
        )
        total = part if total is None else total + part
    return total.astype(jnp.bfloat16)


def local(reps, n, tps, stream_in, mix_gain, lin_weight, branch_weight, lin_taps, rate_blocks, admit_blocks,
          decay_logit, mix_out_gain, out_weight, ffn_gain, gate_weight, up_weight, gate_taps, up_taps, down_weight):
    own = stream_in[0]
    length, share = own.shape
    tp = lax.axis_index("tp")
    flip = [(i, 1 - i) for i in range(2)]

    def features(mine):
        if tps == 2:
            theirs = lax.ppermute(mine, "tp", flip)
            pair = jnp.where(tp == 0, jnp.stack([mine, theirs]), jnp.stack([theirs, mine]))
            return pair
        return lax.all_gather(mine, "tp", axis=0)

    def normed_blocks(mine, gain):
        pair = features(mine).astype(jnp.float32)
        mean_sq = jnp.sum(pair * pair, axis=(0, 2), keepdims=True) / (tps * share)
        y = (pair * lax.rsqrt(mean_sq + EPS) * gain.reshape(tps, 1, share)).astype(jnp.bfloat16)
        y = y.reshape(tps, length, n // tps, (tps * share) // n)
        return y.transpose(0, 2, 1, 3).reshape(n, length, (tps * share) // n)

    def scatter(left, gathered):
        per = n // tps
        if gathered[0][0] == "all":
            part = jnp.dot(left, gathered[0][2], preferred_element_type=jnp.float32).astype(jnp.bfloat16)
            return spread(part.reshape(length, tps, share).transpose(1, 0, 2))
        stack = jnp.zeros((n, length, gathered[0][2].shape[1]), jnp.bfloat16)
        for _, owner, shard in gathered:
            part = jnp.dot(left, shard, preferred_element_type=jnp.float32).astype(jnp.bfloat16)
            stack = lax.dynamic_update_index_in_dim(stack, part, owner, 0)
        stack = stack.reshape(tps, per, length, -1).transpose(0, 2, 1, 3).reshape(tps, length, share)
        return spread(stack)

    def spread(stack):
        if tps == 2:
            mine = lax.dynamic_index_in_dim(stack, tp, 0, keepdims=False)
            other = lax.ppermute(lax.dynamic_index_in_dim(stack, 1 - tp, 0, keepdims=False), "tp", flip)
            return mine.astype(jnp.float32) + other.astype(jnp.float32)
        return lax.psum_scatter(stack, "tp", scatter_dimension=0, tiled=False).astype(jnp.float32)

    def gather(w, sign, name, axis=0):
        if n > CHAIN_LIMIT:
            return [("all", None, lax.all_gather(w, "fs", axis=axis, tiled=True))]
        return chain_gather(w, reps, n, sign, name)

    lin_all = gather(lin_weight, 1, "g_lin")
    branch_all = gather(branch_weight, -1, "g_branch")
    out_all = gather(out_weight, 1, "g_out", 1)
    gate_all = gather(gate_weight, 1, "g_gate")
    up_all = gather(up_weight, -1, "g_up")
    down_all = gather(down_weight, -1, "g_down", 1)

    blocks = normed_blocks(own, mix_gain)
    linear = by_rows(blocks, lin_all)
    branch = by_rows(blocks, branch_all)
    late = (gate_all, up_all, down_all)
    linear, branch = tie((linear, branch), late, ("m1",))
    slope = (-GATE_SCALE * jax.nn.softplus(-decay_logit)).reshape(1, -1)
    mixed = mixer(linear, branch, lin_taps, rate_blocks, admit_blocks, slope, mix_out_gain.reshape(1, -1))
    mixed = tie(mixed, late, ("m2", "o1"))
    middle = (own.astype(jnp.float32) + scatter(mixed, out_all)).astype(jnp.bfloat16)
    middle = tie(middle, late, ("m3", "x2"))
    blocks2 = normed_blocks(middle, ffn_gain)
    gate_pre = by_rows(blocks2, gate_all)
    up_pre = by_rows(blocks2, up_all)
    hidden = ffn_gate(gate_pre, up_pre, gate_taps, up_taps)
    result = (middle.astype(jnp.float32) + scatter(hidden, down_all)).astype(jnp.bfloat16)
    return result[None]


def solution(mesh):
    placed = (
        P(("rep", "fs"), None, "tp"),
        P(),
        P("fs", "tp"),
        P("fs", "tp"),
        P(None, "tp"),
        P("tp", None, None),
        P("tp", None, None),
        P("tp"),
        P("tp"),
        P("tp", "fs"),
        P(),
        P("fs", "tp"),
        P("fs", "tp"),
        P(None, "tp"),
        P(None, "tp"),
        P("tp", "fs"),
    )
    body = functools.partial(local, mesh.shape["rep"], mesh.shape["fs"], mesh.shape["tp"])
    return jax.shard_map(
        body, mesh=mesh, in_specs=placed, out_specs=P(("rep", "fs"), None, "tp"), check_vma=False
    )
```
